512 devices in a mesh: sp: 128 (over z, x, core), tp: 4 (over y).
Axes of the slice: x: 4, y: 4, z: 16, core: 2. Of those that a mesh axis runs over, the one named last changes fastest.
Arguments:
- tokens: bfloat16 [16384, 2048], P(('sp', 'tp')), may hold values from -6 to 6
- input_norm_gain: float32 [2048], replicated, may hold values from 0.1 to 1.9
- convolution_value_weight: bfloat16 [2048, 1024], P('sp', 'tp'), may hold values from -0.125 to 0.125
- convolution_gate_weight: bfloat16 [2048, 1024], P('sp', 'tp'), may hold values from -0.125 to 0.125
- depthwise_filter_taps: float32 [31, 1024], P(None, 'tp'), may hold values from -4 to 4
- channel_norm_gain: float32 [1024], P('tp'), may hold values from 0.1 to 1.9
- channel_norm_bias: float32 [1024], P('tp'), may hold values from -3 to 3
- query_projection_weight: bfloat16 [2048, 1024], P('sp', 'tp'), may hold values from -0.125 to 0.125
- forget_gate_weight: bfloat16 [2048, 1024], P('sp', 'tp'), may hold values from -0.125 to 0.125
- recurrence_value_weight: bfloat16 [2048, 1024], P('sp', 'tp'), may hold values from -0.125 to 0.125
- output_gate_weight: bfloat16 [2048, 1024], P('sp', 'tp'), may hold values from -0.125 to 0.125
- forget_floor_margin: float32 [1024], P('tp'), may hold values from 6.1035156e-06 to 0.1
- decay_jump_terms: float32 [8, 16384], P('tp', 'sp'), may hold values from -0.7 to 0
- head_norm_gain: float32 [1024], P('tp'), may hold values from 0.1 to 1.9
- convolution_output_weight: bfloat16 [1024, 2048], P('tp', 'sp'), may hold values from -0.125 to 0.125
- recurrence_output_weight: bfloat16 [1024, 2048], P('tp', 'sp'), may hold values from -0.125 to 0.125
Outputs:
- mixed: bfloat16 [16384, 2048], P(('sp', 'tp'))
The draws below stay inside these ranges and needn't reach their ends.
All inputs are finite; a program needn't handle non-finite values.
Results may differ from the reference program's by a relative error of at most 0.015.
Values may be sent and summed in bfloat16 or wider, within the bound.
A program may use at most 64 MiB of HBM per device.

```python
import math
import jax
import jax.numpy as jnp
from jax import lax

D = 2048
CONV_CH = 1024
CONV_W = 31
HG_HEADS = 8
HG_DK = 128
HG_DV = 128
HG_BLOCK = 64
TOK_DEV = 128
TOKENS = 16384
N_TP = 4


def draw_depthwise_filter_taps(key, part):
    noise_key, scale_key = jax.random.split(key, 2)
    channel = jnp.arange(CONV_CH, dtype=jnp.float32) / CONV_CH
    jitter = jax.random.uniform(scale_key, (CONV_CH,), jnp.float32, -1.15, 1.15)
    scales = jnp.exp(math.log(3.0) * channel + jitter) / 3.0
    noise_draw = jax.random.normal(noise_key, (CONV_W, CONV_CH), jnp.float32)
    return jnp.clip(noise_draw * scales / math.sqrt(CONV_W), -4.0, 4.0)


def draw_forget_floor_margin(key, part):
    order_key, slow_key, fast_key = jax.random.split(key, 3)
    order = jax.random.permutation(order_key, HG_HEADS)
    slow_head = jnp.repeat(order < HG_HEADS // 2, HG_DK)
    slow_gap = jnp.exp(jax.random.uniform(slow_key, (HG_HEADS * HG_DK,), jnp.float32, math.log(0.1), math.log(0.5))) / TOKENS
    fast_gap = jnp.exp(jax.random.uniform(fast_key, (HG_HEADS * HG_DK,), jnp.float32, math.log(0.03), math.log(0.1)))
    return jnp.where(slow_head, slow_gap, fast_gap)


def draw_decay_jump_terms(key, part):
    rate_key, place_key, depth_key = jax.random.split(key, 3)
    block_total = TOKENS // TOK_DEV
    third = TOKENS // 3
    rates = jnp.exp(jax.random.uniform(rate_key, (HG_HEADS, block_total), jnp.float32, math.log(0.15), math.log(0.6))) / TOKENS
    decay_depths = jnp.log(jax.random.uniform(depth_key, (HG_HEADS, 2), jnp.float32, 0.55, 0.8))
    place_indices = jax.random.randint(place_key, (HG_HEADS, 2), 0, third) + jnp.arange(2)[None, :] * third
    steady_decay = -jnp.repeat(rates, TOK_DEV, axis=1)
    position_indices = jnp.arange(TOKENS)
    decay_jumps = jnp.sum(jnp.where(position_indices[None, None, :] == place_indices[:, :, None], decay_depths[:, :, None], 0.0), axis=1)
    return steady_decay + decay_jumps


def shard_levels(stream_key, extent, cuts, low, high):
    level, own = 1.0, jax.random.fold_in(stream_key, 6)
    for axis_at, shards_of in cuts:
        draws = jnp.exp(jax.random.uniform(jax.random.fold_in(own, axis_at), (shards_of,), jnp.float32, low / len(cuts), high / len(cuts)))
        level = level * jnp.repeat(draws, extent[axis_at] // shards_of).reshape([-1 if axis == axis_at else 1 for axis in range(len(extent))])
    return level


def scatter_about(rng, extent, scale, bound, cuts=(), held_as=jnp.bfloat16):
    loudness = shard_levels(rng, extent, cuts, -0.22, 0.18) if cuts else 1.0
    entries = jax.random.normal(rng, extent, jnp.float32) * scale * loudness
    return jnp.minimum(jnp.maximum(entries, -bound), bound).astype(held_as)


def setup_inputs(seed: int = 0) -> dict:
    splits = jax.random.split(jax.random.key(seed), 17)
    tokens = scatter_about(splits[0], (TOKENS, D), 1.0, 6.0, ((0, 512),))
    input_norm_gain = jnp.clip(1.0 + 0.18 * jax.random.normal(splits[1], (D,), jnp.float32), 0.1, 1.9)
    convolution_value_weight = scatter_about(splits[2], (D, CONV_CH), D ** -0.5, 0.125, ((0, 128), (1, 4)))
    convolution_gate_weight = scatter_about(splits[3], (D, CONV_CH), D ** -0.5, 0.125, ((0, 128), (1, 4)))
    depthwise_filter_taps = draw_depthwise_filter_taps(jax.random.fold_in(splits[16], 71), 0)
    channel_norm_gain = jnp.clip(1.0 + 0.18 * jax.random.normal(splits[5], (CONV_CH,), jnp.float32), 0.1, 1.9)
    channel_norm_bias = scatter_about(splits[6], (CONV_CH,), 0.5, 3.0, ((0, 4),), jnp.float32)
    query_projection_weight = scatter_about(splits[7], (D, HG_HEADS * HG_DK), D ** -0.5, 0.125, ((0, 128), (1, 4)))
    forget_gate_weight = scatter_about(splits[8], (D, HG_HEADS * HG_DK), D ** -0.5, 0.125, ((0, 128), (1, 4)))
    recurrence_value_weight = scatter_about(splits[9], (D, HG_HEADS * HG_DV), D ** -0.5, 0.125, ((0, 128), (1, 4)))
    output_gate_weight = scatter_about(splits[10], (D, HG_HEADS * HG_DV), D ** -0.5, 0.125, ((0, 128), (1, 4)))
    forget_floor_margin = draw_forget_floor_margin(jax.random.fold_in(splits[16], 71), 0)
    decay_jump_terms = draw_decay_jump_terms(jax.random.fold_in(splits[16], 71), 0)
    head_norm_gain = jnp.clip(1.0 + 0.18 * jax.random.normal(splits[13], (HG_HEADS * HG_DV,), jnp.float32), 0.1, 1.9)
    convolution_output_weight = scatter_about(splits[14], (CONV_CH, D), (CONV_CH + HG_HEADS * HG_DV) ** -0.5, 0.125, ((0, 4), (1, 128)))
    recurrence_output_weight = scatter_about(splits[15], (HG_HEADS * HG_DV, D), (CONV_CH + HG_HEADS * HG_DV) ** -0.5, 0.125, ((0, 4), (1, 128)))
    return {"tokens": tokens, "input_norm_gain": input_norm_gain, "convolution_value_weight": convolution_value_weight, "convolution_gate_weight": convolution_gate_weight, "depthwise_filter_taps": depthwise_filter_taps, "channel_norm_gain": channel_norm_gain, "channel_norm_bias": channel_norm_bias, "query_projection_weight": query_projection_weight, "forget_gate_weight": forget_gate_weight, "recurrence_value_weight": recurrence_value_weight, "output_gate_weight": output_gate_weight, "forget_floor_margin": forget_floor_margin, "decay_jump_terms": decay_jump_terms, "head_norm_gain": head_norm_gain, "convolution_output_weight": convolution_output_weight, "recurrence_output_weight": recurrence_output_weight}


norm_eps = 1e-06
layer_eps = 1e-05
highest_precision = lax.Precision.HIGHEST

def convolve(gated, kernel):
    return lax.conv_general_dilated(gated[None], kernel[:, None, :], (1,), 'VALID', dimension_numbers=('NWC', 'WIO', 'NWC'), feature_group_count=gated.shape[1], precision=highest_precision)[0]

def channel_norm(values, first_sum, second_sum, gain, bias):
    mean_value = first_sum[:, None] / CONV_CH
    variance = second_sum[:, None] / CONV_CH - mean_value * mean_value
    shifted = (values - mean_value) * lax.rsqrt(variance + layer_eps) * gain + bias
    return jax.nn.silu(shifted).astype(jnp.bfloat16)

def gate_factors(query_projected, forget_projected, forget_floor_margin, decay_jump_rows):
    row_total_count = query_projected.shape[0]
    head_total_count = decay_jump_rows.shape[1]
    query_rows = jax.nn.silu(query_projected.astype(jnp.float32))
    log_forget_gate = jnp.logaddexp(jnp.log1p(-forget_floor_margin), jnp.log(forget_floor_margin) + jax.nn.log_sigmoid(forget_projected.astype(jnp.float32)))
    key_gate_values = -jnp.expm1(log_forget_gate)
    log_decay_running = log_forget_gate.reshape(row_total_count, head_total_count, -1) + decay_jump_rows[:, :, None]
    return (query_rows.reshape(row_total_count, head_total_count, -1), key_gate_values.reshape(row_total_count, head_total_count, -1), log_decay_running)

def finish(recurrent, gain, outgate_proj):
    row_total_count = recurrent.shape[0]
    scaled = recurrent * lax.rsqrt(lax.optimization_barrier(jnp.mean(recurrent * recurrent, axis=2, keepdims=True)) + norm_eps)
    gated_out = scaled.reshape(row_total_count, -1) * gain * jax.nn.silu(outgate_proj.astype(jnp.float32))
    return gated_out.astype(jnp.bfloat16)

def block_step(recurrence_state, block_parts):
    query_rows, key_gate_values, input_rows, log_decay_running = block_parts
    block_len = query_rows.shape[1]
    cumulative = jnp.cumsum(log_decay_running, axis=1)
    final_decay = cumulative[:, -1:, :]
    query_rows_scaled = query_rows * jnp.exp(cumulative)
    scaled_keys = key_gate_values * jnp.exp(-cumulative)
    final_keys = key_gate_values * jnp.exp(final_decay - cumulative)
    attention_scores = jnp.einsum('htk,hsk->hts', query_rows_scaled, scaled_keys, precision=highest_precision)
    causal = jnp.arange(block_len)[:, None] >= jnp.arange(block_len)[None, :]
    attention_scores = jnp.where(causal[None], attention_scores, 0.0)
    output_rows = jnp.einsum('mby,myx->mbx', attention_scores, input_rows, precision=highest_precision) + jnp.einsum('ufi,uij->ufj', query_rows_scaled, recurrence_state, precision=highest_precision)
    recurrence_state = jnp.exp(final_decay[:, 0, :])[:, :, None] * recurrence_state + jnp.einsum('meg,met->mgt', final_keys, input_rows, precision=highest_precision)
    return (recurrence_state, output_rows)

def reference(tokens, input_norm_gain, convolution_value_weight, convolution_gate_weight, depthwise_filter_taps, channel_norm_gain, channel_norm_bias, query_projection_weight, forget_gate_weight, recurrence_value_weight, output_gate_weight, forget_floor_margin, decay_jump_terms, head_norm_gain, convolution_output_weight, recurrence_output_weight):
    features = tokens.astype(jnp.float32)
    normed = (features * lax.rsqrt(lax.optimization_barrier(jnp.mean(features * features, axis=1, keepdims=True)) + norm_eps) * input_norm_gain).astype(jnp.bfloat16)

    def project(weight):
        return jnp.dot(normed, weight, preferred_element_type=jnp.float32).astype(jnp.bfloat16)
    value_proj = project(convolution_value_weight)
    gate_proj = project(convolution_gate_weight)
    query_projected = project(query_projection_weight)
    forget_projected = project(forget_gate_weight)
    input_proj = project(recurrence_value_weight)
    outgate_proj = project(output_gate_weight)
    gated = value_proj.astype(jnp.float32) * jax.nn.sigmoid(gate_proj.astype(jnp.float32))
    padded = jnp.pad(gated, ((CONV_W - 1, 0), (0, 0)))
    convolved = convolve(padded, depthwise_filter_taps).astype(jnp.bfloat16)
    values = convolved.astype(jnp.float32)
    conv_out = channel_norm(values, lax.optimization_barrier(jnp.sum(values, axis=1)), lax.optimization_barrier(jnp.sum(values * values, axis=1)), channel_norm_gain, channel_norm_bias)
    query_rows, key_gate_values, log_decay_running = gate_factors(query_projected, forget_projected, forget_floor_margin, decay_jump_terms.T)
    input_rows = input_proj.astype(jnp.float32).reshape(TOKENS, HG_HEADS, HG_DV)
    block_count = TOKENS // HG_BLOCK

    def to_blocks(array):
        return array.reshape(block_count, HG_BLOCK, HG_HEADS, -1).transpose(0, 2, 1, 3)
    initial = jnp.zeros((HG_HEADS, HG_DK, HG_DV), jnp.float32)
    scanned = lax.scan(block_step, initial, (to_blocks(query_rows), to_blocks(key_gate_values), to_blocks(input_rows), to_blocks(log_decay_running)))
    recurrent = scanned[1].transpose(0, 2, 1, 3).reshape(TOKENS, HG_HEADS, HG_DV)
    rec_out = finish(recurrent, head_norm_gain, outgate_proj)
    conv_group = CONV_CH // N_TP
    rec_group = HG_HEADS * HG_DV // N_TP
    summed = jnp.zeros((TOKENS, D), jnp.float32)
    for group in range(N_TP):
        conv_slice = slice(group * conv_group, (group + 1) * conv_group)
        rec_slice = slice(group * rec_group, (group + 1) * rec_group)
        partial_sum = jnp.dot(conv_out[:, conv_slice], convolution_output_weight[conv_slice], preferred_element_type=jnp.float32) + jnp.dot(rec_out[:, rec_slice], recurrence_output_weight[rec_slice], preferred_element_type=jnp.float32)
        summed = summed + lax.optimization_barrier(partial_sum.astype(jnp.bfloat16)).astype(jnp.float32)
    return summed.astype(jnp.bfloat16)
```

```python
import jax
import jax.numpy as jnp
from jax import lax
from jax.experimental import pallas as pl
from jax.experimental.pallas import tpu as pltpu
from jax.sharding import Mesh
from jax.sharding import PartitionSpec as P

D = 2048
CONV_CH = 1024
CONV_W = 31
BLOCK = 64
ROWS = 16
TOK = 32
CHIP_TOK = 256
Z, X, C, Y = 16, 4, 2, 4
SP = ("sp_0", "sp_1", "sp_2")
SP_TP = ("sp_0", "sp_1", "sp_2", "tp")
MESH = pl.DeviceIdType.MESH
F32 = jnp.float32
BF16 = jnp.bfloat16
HIGH = lax.Precision.HIGHEST

norm_eps = 1e-06
layer_eps = 1e-05

FORGET, INPUT, QUERY, OUTGATE, VALUE, GATE, CONV_OUT, REC_OUT = range(8)


def dot(a, b, dims, precision=None):
    return lax.dot_general(
        a, b, ((dims[:1], dims[1:]), ((), ())), precision=precision, preferred_element_type=F32
    )


def silu(v):
    return v * jax.nn.sigmoid(v)


def kernel(
    tokens, w_forget, w_input, w_query, w_outgate, w_value, w_gate, w_conv_out, w_rec_out,
    gain, taps, cn_gain, cn_bias, margin, jumps, head_gain,
    out,
    W, Xr, Xn, acc, jbuf, jrecv, hsend, hrecv, gext, conv, stat_s, stat_r,
    qt, inner, starts, p1s, p1r, p2s, p2r, p3s, p3r, AO, ps, pr, po, ss, yr,
    local_sem, wd_s, wd_r, ty_s, ty_r, tp_s, tp_r, j_sem, xa_s, xa_r, xb_s, xb_r, z_s, z_r,
    h_sem, st_s, st_r, p1_s, p1_r, p2_s, p2_r, p3_s, p3_r, o_s, o_r, y_s, y_r,
):
    z = lax.axis_index("sp_0")
    x = lax.axis_index("sp_1")
    c = lax.axis_index("sp_2")
    y = lax.axis_index("tp")
    chip = z * X + x
    weights = (w_forget, w_input, w_query, w_outgate, w_value, w_gate, w_conv_out, w_rec_out)
    half = pl.ds(pl.multiple_of(c * 128, 128), 128)
    other_half = pl.ds(pl.multiple_of((1 - c) * 128, 128), 128)

    def at(dz=0, dx=0, dc=0, dy=0):
        return (
            lax.rem(z + (dz + Z), Z), lax.rem(x + (dx + X), X), lax.rem(c + dc, C),
            lax.rem(y + (dy + Y), Y),
        )

    def send(src, dst, s, r, to):
        return pltpu.make_async_remote_copy(src, dst, s, r, device_id=to, device_id_type=MESH)

    partner = at(dc=1)
    nxt = lax.rem(chip + 1, Z * X)
    prv = lax.rem(chip + Z * X - 1, Z * X)
    next_chip = (nxt // X, lax.rem(nxt, X), c, y)
    prev_chip = (prv // X, lax.rem(prv, X), c, y)

    mine = c * Y + y
    own_tokens = pltpu.make_async_copy(tokens, Xr.at[mine], local_sem.at[8])
    own_tokens.start()
    rows = pl.ds(pl.multiple_of(c * ROWS, ROWS), ROWS)
    own_weights = [
        pltpu.make_async_copy(w.at[:, half], W.at[chip, m, rows], local_sem.at[m])
        for m, w in enumerate(weights)
    ]
    for copy in own_weights:
        copy.start()

    barrier = pltpu.get_barrier_semaphore()
    peers = [partner, next_chip, prev_chip]
    peers += [at(dx=d) for d in range(1, X)]
    peers += [at(dy=d) for d in range(1, Y)] + [at(dy=d, dc=1) for d in range(1, Y)]
    peers += [at(dz=d) for d in range(1, Z)]
    for peer in peers:
        pl.semaphore_signal(barrier, inc=1, device_id=peer, device_id_type=MESH)
    for h in range(2):
        jbuf[h] = jnp.broadcast_to(jumps[h : h + 1, :], (8, 128))
    pl.semaphore_wait(barrier, len(peers))

    sends = []
    for m, w in enumerate(weights):
        copy = send(w.at[:, other_half], W.at[chip, m, rows], wd_s.at[m], wd_r.at[m], partner)
        copy.start()
        sends.append(copy)
    for d in range(1, Y):
        copy = send(tokens, Xr.at[mine], ty_s.at[d], ty_r.at[d], at(dy=d))
        copy.start()
        sends.append(copy)
    copy = send(tokens, Xr.at[mine], tp_s.at[0], tp_r.at[0], partner)
    copy.start()
    sends.append(copy)
    jcopy = send(jbuf.at[1 - c], jrecv, j_sem.at[0], j_sem.at[1], partner)
    jcopy.start()
    sends.append(jcopy)

    prows = pl.ds(pl.multiple_of((1 - c) * ROWS, ROWS), ROWS)
    for m, w in enumerate(weights):
        own_weights[m].wait()
        send(w.at[:, half], W.at[chip, m, prows], wd_s.at[m], wd_r.at[m], partner).wait_recv()

    def z_slot(zo, m):
        if m < 2:
            return W.at[pl.ds(zo * X, X), pl.ds(2 * m, 2)]
        return W.at[zo * X + x, pl.ds(4, 4)]

    def z_copy(way, step, m):
        zo = lax.rem(z + Z + (step - 1) * (1 if way else -1), Z)
        return send(
            z_slot(zo, m), z_slot(zo, m), z_s.at[way, step, m], z_r.at[way, step, m],
            at(dz=-1 if way else 1),
        )

    def z_arrival(way, step, m):
        zo = lax.rem(z + Z + step * (1 if way else -1), Z)
        return send(
            z_slot(zo, m), z_slot(zo, m), z_s.at[way, step, m], z_r.at[way, step, m],
            at(dz=-1 if way else 1),
        )

    def xb_copy(zo, d, own=True):
        slot = W.at[zo * X + (x if own else lax.rem(x + X - d, X)), pl.ds(4, 4)]
        return send(slot, slot, xb_s.at[d, zo], xb_r.at[d, zo], at(dx=d))

    for way in range(2):
        z_copy(way, 1, 2).start()
    slot = W.at[chip, pl.ds(0, 4)]
    for d in range(1, X):
        copy = send(slot, slot, xa_s.at[d], xa_r.at[d], at(dx=d))
        copy.start()
        sends.append(copy)
    for d in range(1, X):
        from_x = W.at[z * X + lax.rem(x + X - d, X), pl.ds(0, 4)]
        send(from_x, from_x, xa_s.at[d], xa_r.at[d], at(dx=d)).wait_recv()
    for m in range(2):
        for way in range(2):
            z_copy(way, 1, m).start()
    for d in range(1, X):
        xb_copy(z, d).start()

    for d in range(1, Y):
        slot = Xr.at[c * Y + lax.rem(y + Y - d, Y)]
        send(tokens, slot, ty_s.at[d], ty_r.at[d], at(dy=d)).wait_recv()
        copy = send(slot, slot, tp_s.at[d], tp_r.at[d], partner)
        copy.start()
        sends.append(copy)

    half_way = Z // 2
    furthest = ((half_way, half_way - 1, half_way), (half_way - 1, half_way, half_way - 1))

    def ring_step(step, last):
        for m in (2, 0, 1):
            for way in range(2):
                if last and furthest[way][m] < half_way:
                    continue
                z_arrival(way, step, m).wait_recv()
                if not last:
                    z_copy(way, step + 1, m).start()
                if m == 2:
                    zo = lax.rem(z + Z + step * (1 if way else -1), Z)
                    for d in range(1, X):
                        xb_copy(zo, d).start()

    def inner_step(step, carry):
        ring_step(step, False)
        return carry

    lax.fori_loop(1, half_way - 1, inner_step, 0)
    for m in (2, 0, 1):
        for way in range(2):
            step = half_way - 1
            z_arrival(way, step, m).wait_recv()
            if furthest[way][m] == half_way:
                z_copy(way, half_way, m).start()
            if m == 2:
                zo = lax.rem(z + Z + step * (1 if way else -1), Z)
                for d in range(1, X):
                    xb_copy(zo, d).start()

    own_tokens.wait()
    for d in range(Y):
        slot = Xr.at[(1 - c) * Y + lax.rem(y + Y - d, Y)]
        send(slot, slot, tp_s.at[d], tp_r.at[d], partner).wait_recv()

    def norm_body(i, carry):
        v = Xr[i // 2, pl.ds(pl.multiple_of(lax.rem(i, 2) * 16, 16), 16), :].astype(F32)
        v = v * lax.rsqrt(jnp.mean(v * v, axis=1, keepdims=True) + norm_eps) * gain[...]
        v = v.astype(BF16)
        for k in range(8):
            Xn[k, pl.ds(pl.multiple_of(i * 16, 16), 16), :] = v[:, k * 256 : (k + 1) * 256]
        return carry

    lax.fori_loop(0, CHIP_TOK // 16, norm_body, 0)
    acc[...] = jnp.zeros_like(acc)

    ring_step(half_way, True)

    def x_wait(zo, carry):
        for d in range(1, X):
            xb_copy(zo, d, own=False).wait_recv()
        return carry

    lax.fori_loop(0, Z, x_wait, 0)

    def weight_block(k, m):
        return W[pl.ds(k * 8, 8), m].reshape(256, 128)

    def project(k, carry):
        xk = Xn[k]
        for p in range(3):
            wk = jnp.concatenate([weight_block(k, 2 * p), weight_block(k, 2 * p + 1)], axis=1)
            acc[:, p * 256 : (p + 1) * 256] += dot(xk, wk, (1, 0))
        return carry

    lax.fori_loop(0, 8, project, 0)

    def projected(m, rows):
        return acc[rows, m * 128 : (m + 1) * 128].astype(BF16)

    last_rows = pl.ds(CHIP_TOK - 32, 32)
    hsend[0] = projected(VALUE, last_rows)
    hsend[1] = projected(GATE, last_rows)
    halo = send(hsend, hrecv, h_sem.at[0], h_sem.at[1], next_chip)
    halo.start()
    sends.append(halo)

    jcopy.wait_recv()
    row_at = lax.broadcasted_iota(jnp.int32, (BLOCK, BLOCK), 0)
    col_at = lax.broadcasted_iota(jnp.int32, (BLOCK, BLOCK), 1)
    causal = row_at >= col_at
    lower = causal.astype(F32)
    own_jump = jnp.broadcast_to(jbuf[c][0:1], (128, 128)).T
    far_jump = jnp.broadcast_to(jrecv[0:1], (128, 128)).T
    first = c == 0
    jump_of = (jnp.where(first, own_jump, far_jump), jnp.where(first, far_jump, own_jump))
    mar = margin[:, half]
    state = jnp.zeros((128, 128), F32)
    total = jnp.zeros((1, 128), F32)
    before = []
    for b in range(CHIP_TOK // BLOCK):
        blk = slice(b * BLOCK, (b + 1) * BLOCK)
        f = projected(FORGET, blk).astype(F32)
        v = projected(INPUT, blk)
        q = silu(projected(QUERY, blk).astype(F32))
        key = mar * jax.nn.sigmoid(-f)
        kept = 1.0 - key
        log_forget = jnp.where(kept == 1.0, -key, jnp.log(kept) * (key / (1.0 - kept)))
        jb = jump_of[b // 2][(b % 2) * BLOCK : (b % 2 + 1) * BLOCK]
        cum = dot(lower, log_forget + jb, (1, 0), HIGH)
        fin = cum[BLOCK - 1 : BLOCK, :]
        q_t = (q * jnp.exp(cum)).astype(BF16)
        k_t = (key * jnp.exp(-cum)).astype(BF16)
        k_f = (key * jnp.exp(fin - cum)).astype(BF16)
        scores = jnp.where(causal, dot(q_t, k_t, (1, 1)), 0.0).astype(BF16)
        inner[blk, :] = dot(scores, v, (1, 0))
        qt[blk, :] = q_t
        starts[b] = state
        before.append(total)
        state = jnp.exp(fin) * state + dot(v, k_f, (0, 0))
        total = total + fin

    upper8 = lax.broadcasted_iota(jnp.int32, (16, 128), 0) < 8

    def pack_decay(a):
        hi = a.astype(BF16).astype(F32)
        return jnp.where(upper8, hi, a - hi).astype(BF16)

    def unpack_decay(block):
        block = block.astype(F32)
        return block[0:1] + block[8:9]

    decay_rows = pack_decay(total)
    for j in range(X):
        p1s[j, 0:32, :] = state[32 * j : 32 * (j + 1)].astype(BF16)
        p1s[j, 32:48, :] = decay_rows
    for d in range(1, X):
        j = lax.rem(x + d, X)
        copy = send(p1s.at[j], p1r.at[x], p1_s.at[d], p1_r.at[d], at(dx=d))
        copy.start()
        sends.append(copy)

    halo.wait_recv()
    halo_rows = hrecv[0].astype(F32) * jax.nn.sigmoid(hrecv[1].astype(F32))
    gext[0:32, :] = jnp.where(chip == 0, 0.0, halo_rows)
    for b in range(CHIP_TOK // BLOCK):
        blk = slice(b * BLOCK, (b + 1) * BLOCK)
        gext[32 + b * BLOCK : 32 + (b + 1) * BLOCK, :] = projected(VALUE, blk).astype(
            F32
        ) * jax.nn.sigmoid(projected(GATE, blk).astype(F32))
    tap_rows = taps[:, half]
    for b in range(CHIP_TOK // BLOCK):
        base = gext[b * BLOCK : b * BLOCK + BLOCK + 32, :]
        total_c = jnp.zeros((BLOCK, 128), F32)
        for j in range(CONV_W):
            total_c += tap_rows[j : j + 1] * base[2 + j : 2 + j + BLOCK]
        conv[b * BLOCK : (b + 1) * BLOCK, :] = total_c.astype(BF16).astype(F32)
    top = lax.broadcasted_iota(jnp.int32, (8, 128), 0) < 4
    for h in range(2):
        turned = conv[h * 128 : (h + 1) * 128, :].T
        first_sum = jnp.sum(turned, axis=0, keepdims=True)
        second_sum = jnp.sum(turned * turned, axis=0, keepdims=True)
        stat_s[:, h * 128 : (h + 1) * 128] = jnp.where(top, first_sum, second_sum)
    for dc in range(C):
        for d in range(Y):
            if dc + d:
                i = dc * Y + d
                copy = send(stat_s, stat_r.at[i], st_s.at[i], st_r.at[i], at(dc=dc, dy=d))
                copy.start()
                sends.append(copy)

    for d in range(1, X):
        j = lax.rem(x + X - d, X)
        send(p1s.at[j], p1r.at[j], p1_s.at[d], p1_r.at[d], at(dx=d)).wait_recv()
    p1r[x] = p1s[x]
    state_in = jnp.zeros((32, 128), F32)
    decay_in = jnp.zeros((1, 128), F32)
    ahead = []
    for j in range(X):
        ahead.append((state_in, decay_in))
        a = unpack_decay(p1r[j, 32:48, :])
        state_in = jnp.exp(a) * state_in + p1r[j, 0:32, :].astype(F32)
        decay_in = decay_in + a
    p2s[0:32, :] = state_in.astype(BF16)
    p2s[32:48, :] = pack_decay(decay_in)
    for d in range(1, Z):
        copy = send(p2s, p2r.at[z], p2_s.at[d], p2_r.at[d], at(dz=d))
        copy.start()
        sends.append(copy)

    for dc in range(C):
        for d in range(Y):
            if dc + d:
                i = dc * Y + d
                send(stat_s, stat_r.at[i], st_s.at[i], st_r.at[i], partner).wait_recv()
    sums = stat_s[...]
    for i in range(1, C * Y):
        sums = sums + stat_r[i]
    for h in range(2):
        blk = slice(h * 128, (h + 1) * 128)
        mean = jnp.broadcast_to(sums[0:1, blk], (128, 128)).T / CONV_CH
        square = jnp.broadcast_to(sums[4:5, blk], (128, 128)).T / CONV_CH
        shifted = (conv[blk, :] - mean) * lax.rsqrt(square - mean * mean + layer_eps)
        AO[blk, 0:128] = silu(shifted * cn_gain[:, half] + cn_bias[:, half]).astype(BF16)

    for d in range(1, Z):
        zo = lax.rem(z + Z - d, Z)
        send(p2s, p2r.at[zo], p2_s.at[d], p2_r.at[d], at(dz=d)).wait_recv()

    def over_z(zo, carried):
        a = unpack_decay(p2r[zo, 32:48, :])
        return jnp.exp(a) * carried + p2r[zo, 0:32, :].astype(F32)

    carried = lax.fori_loop(0, z, over_z, jnp.zeros((32, 128), F32))
    for j in range(X):
        p3s[j] = (jnp.exp(ahead[j][1]) * carried + ahead[j][0]).astype(BF16)
    for d in range(1, X):
        j = lax.rem(x + d, X)
        copy = send(p3s.at[j], p3r.at[x], p3_s.at[d], p3_r.at[d], at(dx=d))
        copy.start()
        sends.append(copy)
    for d in range(1, X):
        j = lax.rem(x + X - d, X)
        send(p3s.at[j], p3r.at[j], p3_s.at[d], p3_r.at[d], at(dx=d)).wait_recv()
    p3r[x] = p3s[x]
    incoming = p3r[...].astype(F32).reshape(128, 128)
    for b in range(CHIP_TOK // BLOCK):
        blk = slice(b * BLOCK, (b + 1) * BLOCK)
        start = (starts[b] + jnp.exp(before[b]) * incoming).astype(BF16)
        rec = inner[blk, :] + dot(qt[blk, :], start, (1, 1))
        rec = rec * lax.rsqrt(jnp.mean(rec * rec, axis=1, keepdims=True) + norm_eps)
        rec = rec * head_gain[:, half] * silu(projected(OUTGATE, blk).astype(F32))
        AO[blk, 128:256] = rec.astype(BF16)

    keep = pl.ds(pl.multiple_of(c * 128, 128), 128)
    give = pl.ds(pl.multiple_of((1 - c) * 128, 128), 128)

    def out_copy(n):
        return send(ps.at[n], pr.at[n], o_s.at[n], o_r.at[n], partner)

    def out_body(n, carry):
        wn = jnp.concatenate([weight_block(n, CONV_OUT), weight_block(n, REC_OUT)], axis=1)
        ps[n] = dot(AO[give, :], wn, (1, 1)).astype(BF16)
        po[n] = dot(AO[keep, :], wn, (1, 1))
        out_copy(n).start()
        return carry

    lax.fori_loop(0, 8, out_body, 0)

    def y_copy(g, d):
        part = pl.ds(g * 2, 2)
        j = lax.rem(y + d, Y)
        return send(
            ss.at[part, j], yr.at[d, part], y_s.at[d, g], y_r.at[d, g], at(dy=d)
        )

    for g in range(4):
        for n in (2 * g, 2 * g + 1):
            out_copy(n).wait_recv()
            summed = po[n] + pr[n].astype(F32)
            ss[n] = summed.astype(BF16).reshape(Y, TOK, 256)
        for d in range(1, Y):
            y_copy(g, d).start()
    for g in range(4):
        for d in range(1, Y):
            y_copy(g, d).wait_recv()
        for n in (2 * g, 2 * g + 1):
            mixed = ss[n, y].astype(F32)
            for d in range(1, Y):
                mixed = mixed + yr[d, n].astype(F32)
            out[:, n * 256 : (n + 1) * 256] = mixed.astype(BF16)

    for copy in sends:
        copy.wait_send()

    def z_drain(step, carry):
        for way in range(2):
            for m in range(3):
                z_copy(way, step, m).wait_send()
        return carry

    lax.fori_loop(1, half_way, z_drain, 0)
    for way in range(2):
        for m in range(3):
            if furthest[way][m] == half_way:
                z_copy(way, half_way, m).wait_send()

    def x_drain(zo, carry):
        for d in range(1, X):
            xb_copy(zo, d).wait_send()
        return carry

    lax.fori_loop(0, Z, x_drain, 0)
    for n in range(8):
        out_copy(n).wait_send()
    for g in range(4):
        for d in range(1, Y):
            y_copy(g, d).wait_send()


def per_device(
    tokens,
    input_norm_gain,
    convolution_value_weight,
    convolution_gate_weight,
    depthwise_filter_taps,
    channel_norm_gain,
    channel_norm_bias,
    query_projection_weight,
    forget_gate_weight,
    recurrence_value_weight,
    output_gate_weight,
    forget_floor_margin,
    decay_jump_terms,
    head_norm_gain,
    convolution_output_weight,
    recurrence_output_weight,
):
    hbm = pl.BlockSpec(memory_space=pl.ANY)
    vmem = pl.BlockSpec(memory_space=pltpu.VMEM)
    dma = pltpu.SemaphoreType.DMA
    chips = Z * X
    return pl.pallas_call(
        kernel,
        name="layer",
        out_shape=jax.ShapeDtypeStruct((TOK, D), BF16),
        in_specs=[hbm] * 9 + [vmem] * 7,
        out_specs=vmem,
        scratch_shapes=[
            pltpu.VMEM((chips, 8, 2 * ROWS, 128), BF16),
            pltpu.VMEM((C * Y, TOK, D), BF16),
            pltpu.VMEM((8, CHIP_TOK, 256), BF16),
            pltpu.VMEM((CHIP_TOK, 768), F32),
            pltpu.VMEM((2, 8, 128), F32),
            pltpu.VMEM((8, 128), F32),
            pltpu.VMEM((2, 32, 128), BF16),
            pltpu.VMEM((2, 32, 128), BF16),
            pltpu.VMEM((32 + CHIP_TOK, 128), F32),
            pltpu.VMEM((CHIP_TOK, 128), F32),
            pltpu.VMEM((8, CHIP_TOK), F32),
            pltpu.VMEM((C * Y, 8, CHIP_TOK), F32),
            pltpu.VMEM((CHIP_TOK, 128), BF16),
            pltpu.VMEM((CHIP_TOK, 128), F32),
            pltpu.VMEM((4, 128, 128), F32),
            pltpu.VMEM((X, 48, 128), BF16),
            pltpu.VMEM((X, 48, 128), BF16),
            pltpu.VMEM((48, 128), BF16),
            pltpu.VMEM((Z, 48, 128), BF16),
            pltpu.VMEM((X, 32, 128), BF16),
            pltpu.VMEM((X, 32, 128), BF16),
            pltpu.VMEM((CHIP_TOK, 256), BF16),
            pltpu.VMEM((8, 128, 256), BF16),
            pltpu.VMEM((8, 128, 256), BF16),
            pltpu.VMEM((8, 128, 256), F32),
            pltpu.VMEM((8, Y, TOK, 256), BF16),
            pltpu.VMEM((Y, 8, TOK, 256), BF16),
            dma((9,)),
            dma((8,)), dma((8,)),
            dma((Y,)), dma((Y,)),
            dma((Y,)), dma((Y,)),
            dma((2,)),
            dma((X,)), dma((X,)),
            dma((X, Z)), dma((X, Z)),
            dma((2, Z // 2 + 1, 3)), dma((2, Z // 2 + 1, 3)),
            dma((2,)),
            dma((C * Y,)), dma((C * Y,)),
            dma((X,)), dma((X,)),
            dma((Z,)), dma((Z,)),
            dma((X,)), dma((X,)),
            dma((8,)), dma((8,)),
            dma((Y, 4)), dma((Y, 4)),
        ],
        compiler_params=pltpu.CompilerParams(
            collective_id=0, has_side_effects=True, vmem_limit_bytes=56 * 1024 * 1024
        ),
    )(
        tokens,
        forget_gate_weight,
        recurrence_value_weight,
        query_projection_weight,
        output_gate_weight,
        convolution_value_weight,
        convolution_gate_weight,
        convolution_output_weight.T,
        recurrence_output_weight.T,
        input_norm_gain[None],
        depthwise_filter_taps,
        channel_norm_gain[None],
        channel_norm_bias[None],
        forget_floor_margin[None],
        decay_jump_terms,
        head_norm_gain[None],
    )


def solution(mesh):
    split = Mesh(mesh.devices.reshape(Z, X, C, Y), SP_TP)
    return jax.shard_map(
        per_device,
        mesh=split,
        in_specs=(
            P(SP_TP, None),
            P(),
            P(SP, "tp"),
            P(SP, "tp"),
            P(None, "tp"),
            P("tp"),
            P("tp"),
            P(SP, "tp"),
            P(SP, "tp"),
            P(SP, "tp"),
            P(SP, "tp"),
            P("tp"),
            P("tp", SP),
            P("tp"),
            P("tp", SP),
            P("tp", SP),
        ),
        out_specs=P(SP_TP, None),
        check_vma=False,
    )
```

```python
import jax
import jax.numpy as jnp
from jax import lax
from jax.experimental import pallas as pl
from jax.experimental.pallas import tpu as pltpu
from jax.sharding import Mesh
from jax.sharding import PartitionSpec as P

D = 2048
CONV_CH = 1024
CONV_W = 31
BLOCK = 64
ROWS = 16
TOK = 32
CHIP_TOK = 256
Z, X, C, Y = 16, 4, 2, 4
SP = ("sp_0", "sp_1", "sp_2")
SP_TP = ("sp_0", "sp_1", "sp_2", "tp")
MESH = pl.DeviceIdType.MESH
F32 = jnp.float32
BF16 = jnp.bfloat16
HIGH = lax.Precision.HIGHEST

norm_eps = 1e-06
layer_eps = 1e-05

FORGET, INPUT, OUTGATE, QUERY, VALUE, GATE, CONV_OUT, REC_OUT = range(8)


def dot(a, b, dims, precision=None):
    return lax.dot_general(
        a, b, ((dims[:1], dims[1:]), ((), ())), precision=precision, preferred_element_type=F32
    )


def silu(v):
    return v * jax.nn.sigmoid(v)


def kernel(
    tokens, w_forget, w_input, w_outgate, w_query, w_value, w_gate, w_conv_out, w_rec_out,
    gain_in, taps_in, cn_gain_in, cn_bias_in, margin_in, jumps_in, head_gain_in,
    out,
    W, Xr, Xn, accs, acc, gain, taps, cn_gain, cn_bias, margin, jumps, head_gain,
    jbuf, jrecv, hsend, hrecv, gext, conv, stat_s, stat_r, keys, cums, qt, inner, starts,
    p1s, p1r, p2s, p2r, p3s, p3r, AO, ps, pr, ss, yr, ob,
    local_sem, one_s, z_s, one_r, ty_r, z_r, xb_r, o_r, y_r,
):
    z = lax.axis_index("sp_0")
    x = lax.axis_index("sp_1")
    c = lax.axis_index("sp_2")
    y = lax.axis_index("tp")
    chip = z * X + x
    weights = (w_forget, w_input, w_outgate, w_query, w_value, w_gate, w_conv_out, w_rec_out)
    half = pl.ds(pl.multiple_of(c * 128, 128), 128)
    other_half = pl.ds(pl.multiple_of((1 - c) * 128, 128), 128)

    def at(dz=0, dx=0, dc=0, dy=0):
        return (
            lax.rem(z + (dz + Z), Z), lax.rem(x + (dx + X), X), lax.rem(c + dc, C),
            lax.rem(y + (dy + Y), Y),
        )

    def send(src, dst, s, r, to):
        return pltpu.make_async_remote_copy(src, dst, s, r, device_id=to, device_id_type=MESH)

    partner = at(dc=1)

    def arrived(ref, r):
        send(ref, ref, one_s.at[0], r, partner).wait_recv()

    def left(ref, s):
        send(ref, ref, s, one_r.at[0], partner).wait_send()

    nxt = lax.rem(chip + 1, Z * X)
    prv = lax.rem(chip + Z * X - 1, Z * X)
    next_chip = (nxt // X, lax.rem(nxt, X), c, y)
    prev_chip = (prv // X, lax.rem(prv, X), c, y)

    mine = c * Y + y
    own_tokens = pltpu.make_async_copy(tokens, Xr.at[mine], local_sem.at[0])
    rows = pl.ds(pl.multiple_of(c * ROWS, ROWS), ROWS)
    for m, w in enumerate(weights):
        pltpu.make_async_copy(w.at[:, half], W.at[chip, m, rows], local_sem.at[1]).start()
    own_tokens.start()
    small = ((gain_in, gain), (taps_in, taps), (cn_gain_in, cn_gain), (cn_bias_in, cn_bias),
             (margin_in, margin), (head_gain_in, head_gain), (jumps_in, jumps))
    small = [pltpu.make_async_copy(a, b, local_sem.at[2 + i]) for i, (a, b) in enumerate(small)]
    for copy in small:
        copy.start()

    barrier = pltpu.get_barrier_semaphore()
    peers = [partner, next_chip, prev_chip]
    peers += [at(dx=d) for d in range(1, X)]
    peers += [at(dy=d) for d in range(1, Y)] + [at(dy=d, dc=1) for d in range(1, Y)]
    peers += [at(dz=d) for d in range(1, Z)]
    for peer in peers:
        pl.semaphore_signal(barrier, inc=1, device_id=peer, device_id_type=MESH)
    pl.semaphore_wait(barrier, len(peers))

    for m, w in enumerate(weights):
        send(w.at[:, other_half], W.at[chip, m, rows], one_s.at[0], one_r.at[0], partner).start()
    for d in range(1, Y):
        send(tokens, Xr.at[mine], one_s.at[1], ty_r.at[d], at(dy=d)).start()
    send(tokens, Xr.at[mine], one_s.at[2], one_r.at[1], partner).start()
    own_rows = W.at[chip, :, rows]
    pltpu.make_async_copy(own_rows, own_rows, local_sem.at[1]).wait()
    arrived(W.at[chip, pl.ds(0, 4)], one_r.at[0])

    def z_slot(zo, m):
        if m == 2:
            return W.at[zo * X + x, pl.ds(3, 5)]
        return W.at[pl.ds(zo * X, X), pl.ds(0, 2) if m == 0 else pl.ds(2, 1)]

    def z_row(way, step):
        return lax.rem(z + Z + step * (1 if way else -1), Z)

    def z_copy(way, step, m, zo):
        return send(
            z_slot(zo, m), z_slot(zo, m), z_s.at[m], z_r.at[way, step, m], at(dz=-1 if way else 1)
        )

    def z_send(way, step, m):
        z_copy(way, step, m, z_row(way, step - 1)).start()

    def z_wait(way, step, m):
        z_copy(way, step, m, z_row(way, step)).wait_recv()

    def x_slot(zo, dx):
        return W.at[zo * X + lax.rem(x + X + dx, X), pl.ds(3, 5)]

    def x_half(zo, dx, side):
        return W.at[zo * X + lax.rem(x + X + dx, X), pl.ds(3, 5), pl.ds(side * 16, 16)]

    def x_send(zo):
        for side, dx in ((0, 1), (1, -1)):
            slot = x_slot(zo, 0)
            send(slot, slot, one_s.at[3], xb_r.at[side, zo], at(dx=dx)).start()

    def x_forward(zo):
        for side, dx in ((0, 1), (1, -1)):
            arrived(x_slot(zo, -dx), xb_r.at[side, zo])
            part = x_half(zo, -dx, side)
            send(part, part, one_s.at[4], one_r.at[2], at(dx=dx)).start()

    for way in range(2):
        z_send(way, 1, 2)
    slot = W.at[chip, pl.ds(0, 3)]
    for d in range(1, X):
        send(slot, slot, one_s.at[5], one_r.at[3], at(dx=d)).start()
    x_send(z)
    arrived(W.at[pl.ds(0, 3), pl.ds(0, 3)], one_r.at[3])
    for m in range(2):
        for way in range(2):
            z_send(way, 1, m)

    def row_block(zo, m):
        return W[pl.ds(zo * X, X), m].reshape(128, 128)

    def project_rows(za, zb, first):
        xk = jnp.concatenate([Xn[za], Xn[zb]], axis=1)
        wk = jnp.concatenate(
            [
                jnp.concatenate([row_block(za, m), row_block(zb, m)], axis=0)
                for m in (FORGET, INPUT)
            ],
            axis=1,
        )
        part = dot(xk, wk, (1, 0))
        accs[...] = part if first else accs[...] + part

    half_way = Z // 2
    furthest = ((half_way, half_way - 1, half_way - 1), (half_way - 1, half_way, half_way))
    for step in range(1, half_way):
        for m in (0, 2, 1):
            for way in range(2):
                z_wait(way, step, m)
                if furthest[way][m] > step:
                    z_send(way, step + 1, m)
                if m == 2:
                    x_send(z_row(way, step))
        for way in range(2):
            if way == 0 or step > 1:
                x_forward(z_row(way, step - 1))
        if step == 1:
            for d in range(1, Y):
                slot = Xr.at[c * Y + lax.rem(y + Y - d, Y)]
                arrived(slot, ty_r.at[d])
                send(slot, slot, one_s.at[2], one_r.at[1], partner).start()
            for h in range(2):
                if h == 0:
                    small[6].wait()
                jbuf[h] = jnp.broadcast_to(jumps[h : h + 1, :], (8, 128))
        if step == 2:
            send(jbuf.at[1 - c], jrecv, one_s.at[6], one_r.at[4], partner).start()
            own_tokens.wait()
            small[0].wait()
            arrived(Xr.at[pl.ds(0, 4)], one_r.at[1])

            def norm_body(i, carry):
                at_row = pl.multiple_of(lax.rem(i, 2) * 16, 16)
                v = Xr[i // 2, pl.ds(at_row, 16), :].astype(F32)
                v = v * lax.rsqrt(jnp.mean(v * v, axis=1, keepdims=True) + norm_eps) * gain[...]
                v = v.astype(BF16)
                for k in range(Z):
                    Xn[k, pl.ds(pl.multiple_of(i * 16, 16), 16), :] = v[:, k * 128 : (k + 1) * 128]
                return carry

            lax.fori_loop(0, CHIP_TOK // 16, norm_body, 0)
        if step >= 3:
            for s in (step, step - 2) if step < 5 else (step,):
                project_rows(z_row(0, s), z_row(1, s), s == 3)

    z_wait(0, half_way, 0)
    z_wait(1, half_way, 2)
    far = z_row(0, half_way)
    x_send(far)
    for way in range(2):
        x_forward(z_row(way, half_way - 1))
    project_rows(z, far, False)

    arrived(jrecv, one_r.at[4])
    for copy in small[1:6]:
        copy.wait()
    row_at = lax.broadcasted_iota(jnp.int32, (BLOCK, BLOCK), 0)
    col_at = lax.broadcasted_iota(jnp.int32, (BLOCK, BLOCK), 1)
    causal = row_at >= col_at
    lower = causal.astype(F32)
    own_jump = jnp.broadcast_to(jbuf[c][0:1], (128, 128)).T
    far_jump = jnp.broadcast_to(jrecv[0:1], (128, 128)).T
    first = c == 0
    jump_of = (jnp.where(first, own_jump, far_jump), jnp.where(first, far_jump, own_jump))
    mar = margin[:, half]
    blocks = [slice(b * BLOCK, (b + 1) * BLOCK) for b in range(CHIP_TOK // BLOCK)]
    state = jnp.zeros((128, 128), F32)
    total = jnp.zeros((1, 128), F32)
    before = []
    for b, blk in enumerate(blocks):
        f = accs[blk, 0:128].astype(BF16).astype(F32)
        v = accs[blk, 128:256].astype(BF16)
        key = mar * jax.nn.sigmoid(-f)
        kept = 1.0 - key
        log_forget = jnp.where(kept == 1.0, -key, jnp.log(kept) * (key / (1.0 - kept)))
        jb = jump_of[b // 2][(b % 2) * BLOCK : (b % 2 + 1) * BLOCK]
        cum = dot(lower, log_forget + jb, (1, 0), HIGH)
        fin = cum[BLOCK - 1 : BLOCK, :]
        k_f = (key * jnp.exp(fin - cum)).astype(BF16)
        keys[blk, :] = key
        cums[blk, :] = cum
        starts[b] = state
        before.append(total)
        state = jnp.exp(fin) * state + dot(v, k_f, (0, 0))
        total = total + fin

    upper8 = lax.broadcasted_iota(jnp.int32, (16, 128), 0) < 8

    def pack_decay(a):
        hi = a.astype(BF16).astype(F32)
        return jnp.where(upper8, hi, a - hi).astype(BF16)

    def unpack_decay(block):
        block = block.astype(F32)
        return block[0:1] + block[8:9]

    decay_rows = pack_decay(total)
    for j in range(X):
        p1s[j, 0:32, :] = state[32 * j : 32 * (j + 1)].astype(BF16)
        p1s[j, 32:48, :] = decay_rows
    for d in range(1, X):
        send(p1s.at[lax.rem(x + d, X)], p1r.at[x], one_s.at[7], one_r.at[5], at(dx=d)).start()
    x_forward(far)
    p1r[x] = p1s[x]
    arrived(p1s.at[pl.ds(0, X - 1)], one_r.at[5])
    state_in = jnp.zeros((32, 128), F32)
    decay_in = jnp.zeros((1, 128), F32)
    ahead = []
    for j in range(X):
        ahead.append((state_in, decay_in))
        a = unpack_decay(p1r[j, 32:48, :])
        state_in = jnp.exp(a) * state_in + p1r[j, 0:32, :].astype(F32)
        decay_in = decay_in + a
    p2s[0:32, :] = state_in.astype(BF16)
    p2s[32:48, :] = pack_decay(decay_in)
    for d in range(1, Z):
        send(p2s, p2r.at[z], one_s.at[8], one_r.at[6], at(dz=d)).start()

    z_wait(1, half_way, 1)
    arrived(W.at[pl.ds(0, 10)], one_r.at[2])

    def weight_block(k, m):
        return W[pl.ds(k * 8, 8), m].reshape(256, 128)

    acc[...] = jnp.zeros_like(acc)

    def project(k, carry):
        xk = jnp.concatenate([Xn[2 * k], Xn[2 * k + 1]], axis=1)
        for p in range(2):
            wk = jnp.concatenate(
                [weight_block(k, 2 + 2 * p), weight_block(k, 3 + 2 * p)], axis=1
            )
            acc[:, p * 256 : (p + 1) * 256] += dot(xk, wk, (1, 0))
        return carry

    lax.fori_loop(0, 8, project, 0)

    def projected(m, rows):
        return acc[rows, (m - 2) * 128 : (m - 1) * 128].astype(BF16)

    last_rows = pl.ds(CHIP_TOK - 32, 32)
    hsend[0] = projected(VALUE, last_rows)
    hsend[1] = projected(GATE, last_rows)
    halo = send(hsend, hrecv, one_s.at[9], one_r.at[7], next_chip)
    halo.start()

    for blk in blocks:
        q = silu(projected(QUERY, blk).astype(F32))
        cum = cums[blk, :]
        q_t = (q * jnp.exp(cum)).astype(BF16)
        k_t = (keys[blk, :] * jnp.exp(-cum)).astype(BF16)
        scores = jnp.where(causal, dot(q_t, k_t, (1, 1)), 0.0).astype(BF16)
        inner[blk, :] = dot(scores, accs[blk, 128:256].astype(BF16), (1, 0))
        qt[blk, :] = q_t

    for blk in blocks:
        gext[32 + blk.start : 32 + blk.stop, :] = projected(VALUE, blk).astype(
            F32
        ) * jax.nn.sigmoid(projected(GATE, blk).astype(F32))
    halo.wait_recv()
    halo_rows = hrecv[0].astype(F32) * jax.nn.sigmoid(hrecv[1].astype(F32))
    gext[0:32, :] = jnp.where(chip == 0, 0.0, halo_rows)
    tap_rows = taps[:, half]
    for b, blk in enumerate(blocks):
        base = gext[b * BLOCK : b * BLOCK + BLOCK + 32, :]
        total_c = jnp.zeros((BLOCK, 128), F32)
        for j in range(CONV_W):
            total_c += tap_rows[j : j + 1] * base[2 + j : 2 + j + BLOCK]
        conv[blk, :] = total_c.astype(BF16).astype(F32)
    top = lax.broadcasted_iota(jnp.int32, (8, 128), 0) < 4
    for h in range(2):
        turned = conv[h * 128 : (h + 1) * 128, :].T
        first_sum = jnp.sum(turned, axis=0, keepdims=True)
        second_sum = jnp.sum(turned * turned, axis=0, keepdims=True)
        stat_s[:, h * 128 : (h + 1) * 128] = jnp.where(top, first_sum, second_sum)
    for dc in range(C):
        for d in range(Y):
            if dc + d:
                i = dc * Y + d
                send(
                    stat_s, stat_r.at[i - 1], one_s.at[10], one_r.at[8], at(dc=dc, dy=d)
                ).start()

    arrived(p2r.at[pl.ds(0, Z - 1)], one_r.at[6])

    def over_z(zo, carried):
        a = unpack_decay(p2r[zo, 32:48, :])
        return jnp.exp(a) * carried + p2r[zo, 0:32, :].astype(F32)

    carried = lax.fori_loop(0, z, over_z, jnp.zeros((32, 128), F32))
    for j in range(X):
        p3s[j] = (jnp.exp(ahead[j][1]) * carried + ahead[j][0]).astype(BF16)
    for d in range(1, X):
        send(p3s.at[lax.rem(x + d, X)], p3r.at[x], one_s.at[11], one_r.at[9], at(dx=d)).start()

    arrived(stat_r.at[pl.ds(0, C * Y - 1)], one_r.at[8])
    sums = stat_s[...]
    for i in range(C * Y - 1):
        sums = sums + stat_r[i]
    for h in range(2):
        blk = slice(h * 128, (h + 1) * 128)
        mean = jnp.broadcast_to(sums[0:1, blk], (128, 128)).T / CONV_CH
        square = jnp.broadcast_to(sums[4:5, blk], (128, 128)).T / CONV_CH
        shifted = (conv[blk, :] - mean) * lax.rsqrt(square - mean * mean + layer_eps)
        AO[blk, 0:128] = silu(shifted * cn_gain[:, half] + cn_bias[:, half]).astype(BF16)

    p3r[x] = p3s[x]
    arrived(p3s.at[pl.ds(0, X - 1)], one_r.at[9])
    incoming = p3r[...].astype(F32).reshape(128, 128)
    for b, blk in enumerate(blocks):
        start = (starts[b] + jnp.exp(before[b]) * incoming).astype(BF16)
        rec = inner[blk, :] + dot(qt[blk, :], start, (1, 1))
        rec = rec * lax.rsqrt(jnp.mean(rec * rec, axis=1, keepdims=True) + norm_eps)
        rec = rec * head_gain[:, half] * silu(projected(OUTGATE, blk).astype(F32))
        AO[blk, 128:256] = rec.astype(BF16)

    keep = pl.ds(pl.multiple_of(c * 128, 128), 128)
    give = pl.ds(pl.multiple_of((1 - c) * 128, 128), 128)

    def out_weight(n):
        return jnp.concatenate([weight_block(n, CONV_OUT), weight_block(n, REC_OUT)], axis=1)

    def out_copy(n):
        return send(ps.at[n], pr.at[n], one_s.at[12], o_r.at[n], partner)

    def give_body(n, carry):
        ps[n] = dot(AO[give, :], out_weight(n), (1, 1)).astype(BF16)
        out_copy(n).start()
        return carry

    lax.fori_loop(0, 8, give_body, 0)

    def y_copy(g, d):
        part = pl.ds(g * 2, 2)
        return send(
            ss.at[part, lax.rem(y + d, Y)], yr.at[d - 1, part], one_s.at[13], y_r.at[g], at(dy=d)
        )

    def keep_body(g, carry):
        for i in range(2):
            n = 2 * g + i
            kept_part = dot(AO[keep, :], out_weight(n), (1, 1))
            out_copy(n).wait_recv()
            ss[n] = (kept_part + pr[n].astype(F32)).astype(BF16).reshape(Y, TOK, 256)
        for d in (2, 1, 3):
            y_copy(g, d).start()
        return carry

    lax.fori_loop(0, 4, keep_body, 0)

    for g in range(4):
        arrived(yr.at[pl.ds(0, Y - 1), pl.ds(g * 2, 2)], y_r.at[g])
        for n in (2 * g, 2 * g + 1):
            mixed = ss[n, y].astype(F32)
            for d in range(Y - 1):
                mixed = mixed + yr[d, n].astype(F32)
            ob[:, n * 256 : (n + 1) * 256] = mixed.astype(BF16)
        cols = pl.ds(g * 512, 512)
        pltpu.make_async_copy(ob.at[:, cols], out.at[:, cols], local_sem.at[9]).start()

    left(W.at[0, pl.ds(0, 4)], one_s.at[0])
    left(Xr.at[pl.ds(0, 3)], one_s.at[1])
    left(Xr.at[pl.ds(0, 4)], one_s.at[2])
    left(W.at[pl.ds(0, 20)], one_s.at[3])
    left(W.at[pl.ds(0, 10)], one_s.at[4])
    left(W.at[pl.ds(0, 3), pl.ds(0, 3)], one_s.at[5])
    left(jrecv, one_s.at[6])
    left(p1s.at[pl.ds(0, X - 1)], one_s.at[7])
    left(p2r.at[pl.ds(0, Z - 1)], one_s.at[8])
    left(hsend, one_s.at[9])
    left(stat_r.at[pl.ds(0, C * Y - 1)], one_s.at[10])
    left(p3s.at[pl.ds(0, X - 1)], one_s.at[11])
    left(ps, one_s.at[12])
    left(ss.at[pl.ds(0, 6)], one_s.at[13])
    left(W.at[pl.ds(0, 15)], z_s.at[0])
    left(W.at[pl.ds(0, 15), pl.ds(0, 4)], z_s.at[1])
    left(W.at[pl.ds(0, 15), pl.ds(0, 5)], z_s.at[2])
    pltpu.make_async_copy(ob, out, local_sem.at[9]).wait()


def per_device(
    tokens,
    input_norm_gain,
    convolution_value_weight,
    convolution_gate_weight,
    depthwise_filter_taps,
    channel_norm_gain,
    channel_norm_bias,
    query_projection_weight,
    forget_gate_weight,
    recurrence_value_weight,
    output_gate_weight,
    forget_floor_margin,
    decay_jump_terms,
    head_norm_gain,
    convolution_output_weight,
    recurrence_output_weight,
):
    hbm = pl.BlockSpec(memory_space=pl.ANY)
    dma = pltpu.SemaphoreType.DMA
    chips = Z * X
    return pl.pallas_call(
        kernel,
        name="layer",
        out_shape=jax.ShapeDtypeStruct((TOK, D), BF16),
        in_specs=[hbm] * 16,
        out_specs=hbm,
        scratch_shapes=[
            pltpu.VMEM((chips, 8, 2 * ROWS, 128), BF16),
            pltpu.VMEM((C * Y, TOK, D), BF16),
            pltpu.VMEM((Z, CHIP_TOK, 128), BF16),
            pltpu.VMEM((CHIP_TOK, 256), F32),
            pltpu.VMEM((CHIP_TOK, 512), F32),
            pltpu.VMEM((1, D), F32),
            pltpu.VMEM((CONV_W, 256), F32),
            pltpu.VMEM((1, 256), F32),
            pltpu.VMEM((1, 256), F32),
            pltpu.VMEM((1, 256), F32),
            pltpu.VMEM((2, 128), F32),
            pltpu.VMEM((1, 256), F32),
            pltpu.VMEM((2, 8, 128), F32),
            pltpu.VMEM((8, 128), F32),
            pltpu.VMEM((2, 32, 128), BF16),
            pltpu.VMEM((2, 32, 128), BF16),
            pltpu.VMEM((32 + CHIP_TOK, 128), F32),
            pltpu.VMEM((CHIP_TOK, 128), F32),
            pltpu.VMEM((8, CHIP_TOK), F32),
            pltpu.VMEM((C * Y - 1, 8, CHIP_TOK), F32),
            pltpu.VMEM((CHIP_TOK, 128), F32),
            pltpu.VMEM((CHIP_TOK, 128), F32),
            pltpu.VMEM((CHIP_TOK, 128), BF16),
            pltpu.VMEM((CHIP_TOK, 128), F32),
            pltpu.VMEM((4, 128, 128), F32),
            pltpu.VMEM((X, 48, 128), BF16),
            pltpu.VMEM((X, 48, 128), BF16),
            pltpu.VMEM((48, 128), BF16),
            pltpu.VMEM((Z, 48, 128), BF16),
            pltpu.VMEM((X, 32, 128), BF16),
            pltpu.VMEM((X, 32, 128), BF16),
            pltpu.VMEM((CHIP_TOK, 256), BF16),
            pltpu.VMEM((8, 128, 256), BF16),
            pltpu.VMEM((8, 128, 256), BF16),
            pltpu.VMEM((8, Y, TOK, 256), BF16),
            pltpu.VMEM((Y - 1, 8, TOK, 256), BF16),
            pltpu.VMEM((TOK, D), BF16),
            dma((10,)),
            dma((14,)),
            dma((3,)),
            dma((10,)),
            dma((Y,)),
            dma((2, Z // 2 + 1, 3)),
            dma((2, Z)),
            dma((8,)),
            dma((4,)),
        ],
        compiler_params=pltpu.CompilerParams(
            collective_id=0, has_side_effects=True, vmem_limit_bytes=56 * 1024 * 1024
        ),
    )(
        tokens,
        forget_gate_weight,
        recurrence_value_weight,
        output_gate_weight,
        query_projection_weight,
        convolution_value_weight,
        convolution_gate_weight,
        convolution_output_weight.T,
        recurrence_output_weight.T,
        input_norm_gain[None],
        depthwise_filter_taps,
        channel_norm_gain[None],
        channel_norm_bias[None],
        forget_floor_margin[None],
        decay_jump_terms,
        head_norm_gain[None],
    )


def solution(mesh):
    split = Mesh(mesh.devices.reshape(Z, X, C, Y), SP_TP)
    return jax.shard_map(
        per_device,
        mesh=split,
        in_specs=(
            P(SP_TP, None),
            P(),
            P(SP, "tp"),
            P(SP, "tp"),
            P(None, "tp"),
            P("tp"),
            P("tp"),
            P(SP, "tp"),
            P(SP, "tp"),
            P(SP, "tp"),
            P(SP, "tp"),
            P("tp"),
            P("tp", SP),
            P("tp"),
            P("tp", SP),
            P("tp", SP),
        ),
        out_specs=P(SP_TP, None),
        check_vma=False,
    )
```

```python
import jax
import jax.numpy as jnp
from jax import lax
from jax.experimental import pallas as pl
from jax.experimental.pallas import tpu as pltpu
from jax.sharding import Mesh
from jax.sharding import PartitionSpec as P

D = 2048
CONV_CH = 1024
CONV_W = 31
BLOCK = 64
ROWS = 16
TOK = 32
CHIP_TOK = 256
Z, X, C, Y = 16, 4, 2, 4
SP = ("sp_0", "sp_1", "sp_2")
SP_TP = ("sp_0", "sp_1", "sp_2", "tp")
MESH = pl.DeviceIdType.MESH
F32 = jnp.float32
BF16 = jnp.bfloat16
HIGH = lax.Precision.HIGHEST

norm_eps = 1e-06
layer_eps = 1e-05

FORGET, INPUT, OUTGATE, QUERY, VALUE, GATE, CONV_OUT, REC_OUT = range(8)


def dot(a, b, dims, precision=None):
    return lax.dot_general(
        a, b, ((dims[:1], dims[1:]), ((), ())), precision=precision, preferred_element_type=F32
    )


def silu(v):
    return v * jax.nn.sigmoid(v)


def kernel(
    tokens, w_forget, w_input, w_outgate, w_query, w_value, w_gate, w_conv_out, w_rec_out,
    gain_in, taps_in, cn_gain_in, cn_bias_in, margin_in, jumps_in, head_gain_in,
    out,
    W, Xr, Xn, accs, acc, gain, taps, cn_gain, cn_bias, margin, jumps, head_gain,
    jbuf, jrecv, hsend, hrecv, gext, conv, stat_s, stat_r, wst, keys, cums, qt, inner, starts,
    p1s, p1r, p2s, p2r, p3s, p3r, AO, wo, ps, pr, po, ss, yr, ob,
    local_sem, one_s, z_s, one_r, ty_r, xa_r, z_r, xb_r, o_r, y_r,
):
    z = lax.axis_index("sp_0")
    x = lax.axis_index("sp_1")
    c = lax.axis_index("sp_2")
    y = lax.axis_index("tp")
    chip = z * X + x
    weights = (w_forget, w_input, w_outgate, w_query, w_value, w_gate, w_conv_out, w_rec_out)
    half = pl.ds(pl.multiple_of(c * 128, 128), 128)
    other_half = pl.ds(pl.multiple_of((1 - c) * 128, 128), 128)

    def at(dz=0, dx=0, dc=0, dy=0):
        return (
            lax.rem(z + (dz + Z), Z), lax.rem(x + (dx + X), X), lax.rem(c + dc, C),
            lax.rem(y + (dy + Y), Y),
        )

    def send(src, dst, s, r, to):
        return pltpu.make_async_remote_copy(src, dst, s, r, device_id=to, device_id_type=MESH)

    partner = at(dc=1)

    def arrived(ref, r):
        send(ref, ref, one_s.at[0], r, partner).wait_recv()

    def left(ref, s):
        send(ref, ref, s, one_r.at[0], partner).wait_send()

    nxt = lax.rem(chip + 1, Z * X)
    prv = lax.rem(chip + Z * X - 1, Z * X)
    next_chip = (nxt // X, lax.rem(nxt, X), c, y)
    prev_chip = (prv // X, lax.rem(prv, X), c, y)

    mine = c * Y + y
    own_tokens = pltpu.make_async_copy(tokens, Xr.at[mine], local_sem.at[0])
    rows = pl.ds(pl.multiple_of(c * ROWS, ROWS), ROWS)
    stage = [pltpu.make_async_copy(w, wst.at[m], local_sem.at[10]) for m, w in enumerate(weights)]
    for copy in stage:
        copy.start()
    for m, w in enumerate(weights):
        pltpu.make_async_copy(w.at[:, half], W.at[chip, m, rows], local_sem.at[1]).start()
    own_tokens.start()
    small = ((gain_in, gain), (taps_in, taps), (cn_gain_in, cn_gain), (cn_bias_in, cn_bias),
             (margin_in, margin), (head_gain_in, head_gain), (jumps_in, jumps))
    small = [pltpu.make_async_copy(a, b, local_sem.at[2 + i]) for i, (a, b) in enumerate(small)]
    for copy in small:
        copy.start()

    barrier = pltpu.get_barrier_semaphore()
    peers = [partner, next_chip, prev_chip]
    peers += [at(dx=d) for d in range(1, X)]
    peers += [at(dy=d) for d in range(1, Y)] + [at(dy=d, dc=1) for d in range(1, Y)]
    peers += [at(dz=1), at(dz=-1)]
    for peer in peers:
        pl.semaphore_signal(barrier, inc=1, device_id=peer, device_id_type=MESH)
    pltpu.make_async_copy(wst, wst, local_sem.at[10]).wait()
    own_tokens.wait()
    pl.semaphore_wait(barrier, len(peers))

    part = wst.at[:, :, other_half]
    send(part, W.at[chip, :, rows], one_s.at[0], one_r.at[0], partner).start()
    for d in range(1, Y):
        send(Xr.at[mine], Xr.at[mine], one_s.at[1], ty_r.at[d], at(dy=d)).start()
    send(Xr.at[mine], Xr.at[mine], one_s.at[2], one_r.at[1], partner).start()
    own_rows = W.at[chip, :, rows]
    pltpu.make_async_copy(own_rows, own_rows, local_sem.at[1]).wait()
    arrived(W.at[chip, pl.ds(0, 4)], one_r.at[0])

    def z_slot(zo, m):
        if m >= X:
            return W.at[zo * X + x, pl.ds(3, 3) if m == X else pl.ds(6, 2)]
        return W.at[zo * X + lax.rem(x + m, X), pl.ds(0, 3)]

    def z_row(way, step):
        return lax.rem(z + Z + step * (1 if way else -1), Z)

    def z_copy(way, step, m, zo):
        sem = z_s.at[0 if m < X else m - X + 1]
        return send(
            z_slot(zo, m), z_slot(zo, m), sem, z_r.at[way, step, m], at(dz=-1 if way else 1)
        )

    def z_send(way, step, m):
        z_copy(way, step, m, z_row(way, step - 1)).start()

    def z_wait(way, step, m):
        z_copy(way, step, m, z_row(way, step)).wait_recv()

    def x_slot(zo, dx):
        return W.at[zo * X + lax.rem(x + X + dx, X), pl.ds(3, 5)]

    def x_half(zo, dx, side):
        return W.at[zo * X + lax.rem(x + X + dx, X), pl.ds(3, 5), pl.ds(side * 16, 16)]

    def x_send(zo):
        for side, dx in ((0, 1), (1, -1)):
            slot = x_slot(zo, 0)
            send(slot, slot, one_s.at[3], xb_r.at[side, zo], at(dx=dx)).start()

    def x_forward(zo):
        for side, dx in ((0, 1), (1, -1)):
            arrived(x_slot(zo, -dx), xb_r.at[side, zo])
            part = x_half(zo, -dx, side)
            send(part, part, one_s.at[4], one_r.at[2], at(dx=dx)).start()

    slot = W.at[chip, pl.ds(0, 3)]
    for d in (1, X - 1, 2):
        send(slot, slot, one_s.at[5], xa_r.at[d], at(dx=d)).start()
    for m in (0, X, X + 1):
        for way in range(2):
            z_send(way, 1, m)
    x_send(z)
    for d in (1, X - 1, 2):
        arrived(W.at[z * X + lax.rem(x + X - d, X), pl.ds(0, 3)], xa_r.at[d])
        for way in range(2):
            z_send(way, 1, X - d)

    def norm_body(i, carry):
        at_row = pl.multiple_of(lax.rem(i, 2) * 16, 16)
        v = Xr[i // 2, pl.ds(at_row, 16), :].astype(F32)
        v = v * lax.rsqrt(jnp.mean(v * v, axis=1, keepdims=True) + norm_eps) * gain[...]
        v = v.astype(BF16)
        for k in range(Z):
            Xn[k, pl.ds(pl.multiple_of(i * 16, 16), 16), :] = v[:, k * 128 : (k + 1) * 128]
        return carry

    def row_block(zo, m):
        return W[pl.ds(zo * X, X), m].reshape(128, 128)

    def project_rows(za, zb, first):
        xk = jnp.concatenate([Xn[za], Xn[zb]], axis=1)
        wk = jnp.concatenate(
            [
                jnp.concatenate([row_block(za, m), row_block(zb, m)], axis=0)
                for m in (FORGET, INPUT)
            ],
            axis=1,
        )
        part = dot(xk, wk, (1, 0))
        accs[...] = part if first else accs[...] + part

    half_way = Z // 2
    far_way = (0, 1, 0, 1, 0, 1)
    for step in range(1, half_way):
        for m in (0, 4, 3, 5, 1, 2):
            for way in range(2):
                z_wait(way, step, m)
                if step + 1 < half_way or far_way[m] == way:
                    z_send(way, step + 1, m)
                if m == 5:
                    x_send(z_row(way, step))
        for way in range(2):
            if way == 0 or step > 1:
                x_forward(z_row(way, step - 1))
        if step == 1:
            for d in range(1, Y):
                slot = Xr.at[c * Y + lax.rem(y + Y - d, Y)]
                arrived(slot, ty_r.at[d])
                send(slot, slot, one_s.at[2], one_r.at[1], partner).start()
            for h in range(2):
                if h == 0:
                    small[6].wait()
                jbuf[h] = jnp.broadcast_to(jumps[h : h + 1, :], (8, 128))
        if step == 2:
            send(jbuf.at[1 - c], jrecv, one_s.at[6], one_r.at[4], partner).start()
            small[0].wait()
            arrived(Xr.at[pl.ds(0, 4)], one_r.at[1])
        if 2 <= step <= 5:
            lax.fori_loop(4 * (step - 2), 4 * (step - 1), norm_body, 0)
        if step >= 6:
            for s in range(3 * step - 17, 3 * step - 14):
                project_rows(z_row(0, s), z_row(1, s), s == 1)
    for m in (0, 4, 3, 5, 1, 2):
        z_wait(far_way[m], half_way, m)
    far = z_row(0, half_way)
    x_send(far)
    for way in range(2):
        x_forward(z_row(way, half_way - 1))
    project_rows(z_row(0, half_way - 1), z_row(1, half_way - 1), False)
    project_rows(z, far, False)

    arrived(jrecv, one_r.at[4])
    for copy in small[1:6]:
        copy.wait()
    row_at = lax.broadcasted_iota(jnp.int32, (BLOCK, BLOCK), 0)
    col_at = lax.broadcasted_iota(jnp.int32, (BLOCK, BLOCK), 1)
    causal = row_at >= col_at
    lower = causal.astype(F32)
    own_jump = jnp.broadcast_to(jbuf[c][0:1], (128, 128)).T
    far_jump = jnp.broadcast_to(jrecv[0:1], (128, 128)).T
    first = c == 0
    jump_of = (jnp.where(first, own_jump, far_jump), jnp.where(first, far_jump, own_jump))
    mar = margin[:, half]
    blocks = [slice(b * BLOCK, (b + 1) * BLOCK) for b in range(CHIP_TOK // BLOCK)]
    state = jnp.zeros((128, 128), F32)
    total = jnp.zeros((1, 128), F32)
    before = []
    for b, blk in enumerate(blocks):
        f = accs[blk, 0:128].astype(BF16).astype(F32)
        v = accs[blk, 128:256].astype(BF16)
        key = mar * jax.nn.sigmoid(-f)
        kept = 1.0 - key
        log_forget = jnp.where(kept == 1.0, -key, jnp.log(kept) * (key / (1.0 - kept)))
        jb = jump_of[b // 2][(b % 2) * BLOCK : (b % 2 + 1) * BLOCK]
        cum = dot(lower, log_forget + jb, (1, 0), HIGH)
        fin = cum[BLOCK - 1 : BLOCK, :]
        k_f = (key * jnp.exp(fin - cum)).astype(BF16)
        keys[blk, :] = key
        cums[blk, :] = cum
        starts[b] = state
        before.append(total)
        state = jnp.exp(fin) * state + dot(v, k_f, (0, 0))
        total = total + fin

    upper4 = lax.broadcasted_iota(jnp.int32, (8, 128), 0) < 4

    def pack_decay(a):
        hi = a.astype(BF16).astype(F32)
        return jnp.where(upper4, hi, a - hi).astype(BF16)

    def unpack_decay(block):
        block = block.astype(F32)
        return block[0:1] + block[4:5]

    decay_rows = pack_decay(total)
    for j in range(X):
        p1s[j, 0:32, :] = state[32 * j : 32 * (j + 1)].astype(BF16)
        p1s[j, 32:40, :] = decay_rows
    for d in range(1, X):
        send(p1s.at[lax.rem(x + d, X)], p1r.at[x], one_s.at[7], one_r.at[5], at(dx=d)).start()
    x_forward(far)
    p1r[x] = p1s[x]
    arrived(p1s.at[pl.ds(0, X - 1)], one_r.at[5])
    state_in = jnp.zeros((32, 128), F32)
    decay_in = jnp.zeros((1, 128), F32)
    ahead = []
    for j in range(X):
        ahead.append((state_in, decay_in))
        a = unpack_decay(p1r[j, 32:40, :])
        state_in = jnp.exp(a) * state_in + p1r[j, 0:32, :].astype(F32)
        decay_in = decay_in + a
    p2s[0:32, :] = state_in.astype(BF16)
    p2s[32:40, :] = pack_decay(decay_in)
    for d in range(1, Z):
        send(p2s, p2r.at[z], one_s.at[8], one_r.at[6], at(dz=d)).start()

    arrived(W.at[pl.ds(0, 10)], one_r.at[2])

    def weight_block(k, m):
        return W[pl.ds(k * 8, 8), m].reshape(256, 128)

    acc[...] = jnp.zeros_like(acc)

    def project(k, carry):
        xk = jnp.concatenate([Xn[2 * k], Xn[2 * k + 1]], axis=1)
        for p in range(2):
            wk = jnp.concatenate(
                [weight_block(k, 2 + 2 * p), weight_block(k, 3 + 2 * p)], axis=1
            )
            acc[:, p * 256 : (p + 1) * 256] += dot(xk, wk, (1, 0))
        return carry

    lax.fori_loop(0, 8, project, 0)

    def projected(m, rows):
        return acc[rows, (m - 2) * 128 : (m - 1) * 128].astype(BF16)

    last_rows = pl.ds(CHIP_TOK - 32, 32)
    hsend[0] = projected(VALUE, last_rows)
    hsend[1] = projected(GATE, last_rows)
    halo = send(hsend, hrecv, one_s.at[9], one_r.at[7], next_chip)
    halo.start()

    for blk in blocks:
        q = silu(projected(QUERY, blk).astype(F32))
        cum = cums[blk, :]
        q_t = (q * jnp.exp(cum)).astype(BF16)
        k_t = (keys[blk, :] * jnp.exp(-cum)).astype(BF16)
        scores = jnp.where(causal, dot(q_t, k_t, (1, 1)), 0.0).astype(BF16)
        inner[blk, :] = dot(scores, accs[blk, 128:256].astype(BF16), (1, 0))
        qt[blk, :] = q_t

    for blk in blocks:
        gext[32 + blk.start : 32 + blk.stop, :] = projected(VALUE, blk).astype(
            F32
        ) * jax.nn.sigmoid(projected(GATE, blk).astype(F32))
    halo.wait_recv()
    halo_rows = hrecv[0].astype(F32) * jax.nn.sigmoid(hrecv[1].astype(F32))
    gext[0:32, :] = jnp.where(chip == 0, 0.0, halo_rows)
    tap_rows = taps[:, half]
    for b, blk in enumerate(blocks):
        base = gext[b * BLOCK : b * BLOCK + BLOCK + 32, :]
        total_c = jnp.zeros((BLOCK, 128), F32)
        for j in range(CONV_W):
            total_c += tap_rows[j : j + 1] * base[2 + j : 2 + j + BLOCK]
        conv[blk, :] = total_c.astype(BF16).astype(F32)
    top = lax.broadcasted_iota(jnp.int32, (8, 128), 0) < 4
    for h in range(2):
        turned = conv[h * 128 : (h + 1) * 128, :].T
        first_sum = jnp.sum(turned, axis=0, keepdims=True)
        second_sum = jnp.sum(turned * turned, axis=0, keepdims=True)
        stat_s[:, h * 128 : (h + 1) * 128] = jnp.where(top, first_sum, second_sum)
    for dc in range(C):
        for d in range(Y):
            if dc + d:
                i = dc * Y + d
                send(
                    stat_s, stat_r.at[i - 1], one_s.at[10], one_r.at[8], at(dc=dc, dy=d)
                ).start()

    def turn_body(n, carry):
        wo[n, 0:128, :] = weight_block(n, CONV_OUT).T
        wo[n, 128:256, :] = weight_block(n, REC_OUT).T
        return carry

    lax.fori_loop(0, 8, turn_body, 0)

    arrived(p2r.at[pl.ds(0, Z - 1)], one_r.at[6])

    def over_z(zo, carried):
        a = unpack_decay(p2r[zo, 32:40, :])
        return jnp.exp(a) * carried + p2r[zo, 0:32, :].astype(F32)

    carried = lax.fori_loop(0, z, over_z, jnp.zeros((32, 128), F32))
    for j in range(X):
        p3s[j] = (jnp.exp(ahead[j][1]) * carried + ahead[j][0]).astype(BF16)
    for d in range(1, X):
        send(p3s.at[lax.rem(x + d, X)], p3r.at[x], one_s.at[11], one_r.at[9], at(dx=d)).start()

    arrived(stat_r.at[pl.ds(0, C * Y - 1)], one_r.at[8])
    sums = stat_s[...]
    for i in range(C * Y - 1):
        sums = sums + stat_r[i]
    for h in range(2):
        blk = slice(h * 128, (h + 1) * 128)
        mean = jnp.broadcast_to(sums[0:1, blk], (128, 128)).T / CONV_CH
        square = jnp.broadcast_to(sums[4:5, blk], (128, 128)).T / CONV_CH
        shifted = (conv[blk, :] - mean) * lax.rsqrt(square - mean * mean + layer_eps)
        AO[blk, 0:128] = silu(shifted * cn_gain[:, half] + cn_bias[:, half]).astype(BF16)

    p3r[x] = p3s[x]
    arrived(p3s.at[pl.ds(0, X - 1)], one_r.at[9])
    incoming = p3r[...].astype(F32).reshape(128, 128)
    for b, blk in enumerate(blocks):
        start = (starts[b] + jnp.exp(before[b]) * incoming).astype(BF16)
        rec = inner[blk, :] + dot(qt[blk, :], start, (1, 1))
        rec = rec * lax.rsqrt(jnp.mean(rec * rec, axis=1, keepdims=True) + norm_eps)
        rec = rec * head_gain[:, half] * silu(projected(OUTGATE, blk).astype(F32))
        AO[blk, 128:256] = rec.astype(BF16)

    keep = pl.ds(pl.multiple_of(c * 128, 128), 128)
    give = pl.ds(pl.multiple_of((1 - c) * 128, 128), 128)

    def out_copy(n):
        return send(ps.at[n], pr.at[n], one_s.at[12], o_r.at[n], partner)

    def y_copy(g, d):
        part = pl.ds(g * 2, 2)
        return send(
            ss.at[part, lax.rem(y + d, Y)], yr.at[d - 1, part], one_s.at[13], y_r.at[g], at(dy=d)
        )

    def pair_sum(g):
        for n in (2 * g, 2 * g + 1):
            out_copy(n).wait_recv()
            ss[n] = (po[n] + pr[n].astype(F32)).astype(BF16).reshape(Y, TOK, 256)
        for d in (2, 1, 3):
            y_copy(g, d).start()

    def out_body(g, carry):
        for i in range(2):
            n = 2 * g + i
            ps[n] = dot(AO[give, :], wo[n], (1, 0)).astype(BF16)
            out_copy(n).start()
            po[n] = dot(AO[keep, :], wo[n], (1, 0))
        return carry

    for g in range(4):
        out_body(g, 0)
        if g:
            pair_sum(g - 1)
    pair_sum(3)

    left(W.at[0, pl.ds(0, 4)], one_s.at[0])
    left(Xr.at[pl.ds(0, 3)], one_s.at[1])
    left(Xr.at[pl.ds(0, 4)], one_s.at[2])
    left(W.at[pl.ds(0, 20)], one_s.at[3])
    left(W.at[pl.ds(0, 10)], one_s.at[4])
    left(W.at[pl.ds(0, 3), pl.ds(0, 3)], one_s.at[5])
    left(jrecv, one_s.at[6])
    left(p1s.at[pl.ds(0, X - 1)], one_s.at[7])
    left(p2r.at[pl.ds(0, Z - 1)], one_s.at[8])
    left(hsend, one_s.at[9])
    left(stat_r.at[pl.ds(0, C * Y - 1)], one_s.at[10])
    left(p3s.at[pl.ds(0, X - 1)], one_s.at[11])
    left(W.at[pl.ds(0, 60), pl.ds(0, 3)], z_s.at[0])
    left(W.at[pl.ds(0, 15), pl.ds(0, 3)], z_s.at[1])
    left(W.at[pl.ds(0, 15), pl.ds(0, 2)], z_s.at[2])
    for g in range(4):
        arrived(yr.at[pl.ds(0, Y - 1), pl.ds(g * 2, 2)], y_r.at[g])
        for n in (2 * g, 2 * g + 1):
            mixed = ss[n, y].astype(F32)
            for d in range(Y - 1):
                mixed = mixed + yr[d, n].astype(F32)
            ob[:, n * 256 : (n + 1) * 256] = mixed.astype(BF16)
        cols = pl.ds(g * 512, 512)
        pltpu.make_async_copy(ob.at[:, cols], out.at[:, cols], local_sem.at[9]).start()

    left(ps, one_s.at[12])
    left(ss.at[pl.ds(0, 6)], one_s.at[13])
    pltpu.make_async_copy(ob, out, local_sem.at[9]).wait()


def per_device(
    tokens,
    input_norm_gain,
    convolution_value_weight,
    convolution_gate_weight,
    depthwise_filter_taps,
    channel_norm_gain,
    channel_norm_bias,
    query_projection_weight,
    forget_gate_weight,
    recurrence_value_weight,
    output_gate_weight,
    forget_floor_margin,
    decay_jump_terms,
    head_norm_gain,
    convolution_output_weight,
    recurrence_output_weight,
):
    hbm = pl.BlockSpec(memory_space=pl.ANY)
    dma = pltpu.SemaphoreType.DMA
    chips = Z * X
    return pl.pallas_call(
        kernel,
        name="layer",
        out_shape=jax.ShapeDtypeStruct((TOK, D), BF16),
        in_specs=[hbm] * 16,
        out_specs=hbm,
        scratch_shapes=[
            pltpu.VMEM((chips, 8, 2 * ROWS, 128), BF16),
            pltpu.VMEM((C * Y, TOK, D), BF16),
            pltpu.VMEM((Z, CHIP_TOK, 128), BF16),
            pltpu.VMEM((CHIP_TOK, 256), F32),
            pltpu.VMEM((CHIP_TOK, 512), F32),
            pltpu.VMEM((1, D), F32),
            pltpu.VMEM((CONV_W, 256), F32),
            pltpu.VMEM((1, 256), F32),
            pltpu.VMEM((1, 256), F32),
            pltpu.VMEM((1, 256), F32),
            pltpu.VMEM((2, 128), F32),
            pltpu.VMEM((1, 256), F32),
            pltpu.VMEM((2, 8, 128), F32),
            pltpu.VMEM((8, 128), F32),
            pltpu.VMEM((2, 32, 128), BF16),
            pltpu.VMEM((2, 32, 128), BF16),
            pltpu.VMEM((32 + CHIP_TOK, 128), F32),
            pltpu.VMEM((CHIP_TOK, 128), F32),
            pltpu.VMEM((8, CHIP_TOK), F32),
            pltpu.VMEM((C * Y - 1, 8, CHIP_TOK), F32),
            pltpu.VMEM((8, ROWS, 256), BF16),
            pltpu.VMEM((CHIP_TOK, 128), F32),
            pltpu.VMEM((CHIP_TOK, 128), F32),
            pltpu.VMEM((CHIP_TOK, 128), BF16),
            pltpu.VMEM((CHIP_TOK, 128), F32),
            pltpu.VMEM((4, 128, 128), F32),
            pltpu.VMEM((X, 40, 128), BF16),
            pltpu.VMEM((X, 40, 128), BF16),
            pltpu.VMEM((40, 128), BF16),
            pltpu.VMEM((Z, 40, 128), BF16),
            pltpu.VMEM((X, 32, 128), BF16),
            pltpu.VMEM((X, 32, 128), BF16),
            pltpu.VMEM((CHIP_TOK, 256), BF16),
            pltpu.VMEM((8, 256, 256), BF16),
            pltpu.VMEM((8, 128, 256), BF16),
            pltpu.VMEM((8, 128, 256), BF16),
            pltpu.VMEM((8, 128, 256), F32),
            pltpu.VMEM((8, Y, TOK, 256), BF16),
            pltpu.VMEM((Y - 1, 8, TOK, 256), BF16),
            pltpu.VMEM((TOK, D), BF16),
            dma((11,)),
            dma((14,)),
            dma((3,)),
            dma((10,)),
            dma((Y,)),
            dma((X,)),
            dma((2, Z // 2 + 1, 6)),
            dma((2, Z)),
            dma((8,)),
            dma((4,)),
        ],
        compiler_params=pltpu.CompilerParams(
            collective_id=0, has_side_effects=True, vmem_limit_bytes=56 * 1024 * 1024
        ),
    )(
        tokens,
        forget_gate_weight,
        recurrence_value_weight,
        output_gate_weight,
        query_projection_weight,
        convolution_value_weight,
        convolution_gate_weight,
        convolution_output_weight.T,
        recurrence_output_weight.T,
        input_norm_gain[None],
        depthwise_filter_taps,
        channel_norm_gain[None],
        channel_norm_bias[None],
        forget_floor_margin[None],
        decay_jump_terms,
        head_norm_gain[None],
    )


def solution(mesh):
    split = Mesh(mesh.devices.reshape(Z, X, C, Y), SP_TP)
    return jax.shard_map(
        per_device,
        mesh=split,
        in_specs=(
            P(SP_TP, None),
            P(),
            P(SP, "tp"),
            P(SP, "tp"),
            P(None, "tp"),
            P("tp"),
            P("tp"),
            P(SP, "tp"),
            P(SP, "tp"),
            P(SP, "tp"),
            P(SP, "tp"),
            P("tp"),
            P("tp", SP),
            P("tp"),
            P("tp", SP),
            P("tp", SP),
        ),
        out_specs=P(SP_TP, None),
        check_vma=False,
    )
```
